512 devices in a mesh: sp: 32 (over z, core), tp: 16 (over y, x).
Axes of the slice: x: 4, y: 4, z: 16, core: 2. Of those that a mesh axis runs over, the one named last changes fastest.
Arguments:
- residual_signal: bfloat16 [4096, 2048], P(('sp', 'tp')), may hold values from -6 to 6
- prelayer_scaling_factor: float32 [2048], replicated, may hold values from 0.1 to 1.9
- result_adjoint: bfloat16 [4096, 2048], P(('sp', 'tp')), may hold values from -24 to 24
- chosen_specialist_ids: int32 [4096, 2], P('sp'), may hold values from 0 to 31, all different within a row; in each aligned block of 128 rows (0 to 127, 128 to 255, ...) at most 10 rows name the same one
- dispatch_shares: float32 [4096, 2], P('sp'), may hold values from 0.2 to 1
- specialist_valve_matrix: bfloat16 [32, 2048, 2048], P('sp', None, 'tp'), may hold values from -0.125 to 0.125
- specialist_widen_matrix: bfloat16 [32, 2048, 2048], P('sp', None, 'tp'), may hold values from -0.125 to 0.125
- specialist_shrink_matrix: bfloat16 [32, 2048, 2048], P('sp', 'tp'), may hold values from -0.125 to 0.125
- probe_vectors: bfloat16 [4096, 1024], P('sp'), may hold values from -6 to 6
- lookup_vectors: bfloat16 [4096, 1024], P('sp'), may hold values from -1.5 to 1.5
- persistence_scores: bfloat16 [4096, 1024], P('sp'), may hold values from -2 to 8
- group_additional_shrinkage: float32 [4096, 2], P('sp'), may hold values from -4.2 to 0
- content_vectors: bfloat16 [4096, 2, 1024], P('sp', None, 'tp'), may hold values from -6 to 6
- result_valve_scores: bfloat16 [4096, 2, 1024], P('sp', None, 'tp'), may hold values from -6 to 6
- stored_opening_memory: float32 [32, 2, 512, 1024], P('sp', None, None, 'tp'), may hold values from -24 to 24
- result_mapping_matrix: bfloat16 [2048, 2, 1024], P(None, None, 'tp'), may hold values from -0.125 to 0.125
Outputs:
- stream_grad: bfloat16 [4096, 2048], P(('sp', 'tp'))
- gate_grad: bfloat16 [32, 2048, 2048], P('sp', None, 'tp')
- up_grad: bfloat16 [32, 2048, 2048], P('sp', None, 'tp')
- down_grad: bfloat16 [32, 2048, 2048], P('sp', 'tp')
- proj_grad: float32 [2048, 2, 1024], P('sp', None, 'tp')
- query_grad: bfloat16 [4096, 1024], P('sp', 'tp')
- key_grad: bfloat16 [4096, 1024], P('sp', 'tp')
- retain_preact_derivative: float32 [4096, 1024], P('sp', 'tp')
- value_grad: bfloat16 [4096, 2, 1024], P('sp', None, 'tp')
- gate_input_grad: bfloat16 [4096, 2, 1024], P('sp', None, 'tp')
The draws below stay inside these ranges and needn't reach their ends.
Inputs may be any that keep to these rules, and one draw needn't show every extreme that they name: `chosen_specialist_ids`: the 2 experts of a token differ. In each aligned block of 128 tokens no expert is named by more than 10 tokens, a bound that some expert reaches in some block.
All inputs are finite; a program needn't handle non-finite values.
Results may differ from the reference program's by a relative error of at most 0.028.
Values may be sent and summed in bfloat16 or wider, within the bound.
A program may use at most 64 MiB of HBM per device.

```python
import math
import jax
import jax.numpy as jnp
import numpy as np
from jax import lax

D = 2048
FOCUS_GROUPS = 2
FEATURE_DIMS = 512
HEAD_V = 1024
FF = 2048
TOP = 2
PIECE_PLACES = 64
TOK_DEV = 128
CORPUS_SPAN = 4096
EXPERTS = 32
QUERY_CHANNELS = 1024
CAP = 10
FF_PART = 128
HV_PART = 64
N_SP = 32
N_TP = 16


def draw_persistence_scores(key, part):
    channel_count = FOCUS_GROUPS * FEATURE_DIMS
    pick_key, fast_key, span_key, noise_key = jax.random.split(jax.random.fold_in(key, 11), 4)
    picks = jax.random.randint(pick_key, (channel_count,), 0, 20)
    slow_mask = picks < 10
    slow_level = jnp.log(jnp.float32(CORPUS_SPAN) / 25.6)
    fast_level = jax.random.uniform(fast_key, (channel_count,), jnp.float32, -0.5, 1.0)
    levels = jnp.where(slow_mask, slow_level, fast_level)
    span_shift = jnp.repeat(jax.random.uniform(span_key, (CORPUS_SPAN // TOK_DEV, 1), jnp.float32, -0.5, 0.5), TOK_DEV, axis=0)
    noise = jax.random.uniform(noise_key, (CORPUS_SPAN, channel_count), jnp.float32, -1.0, 1.0)
    return (levels[None, :] + span_shift + noise).astype(jnp.bfloat16)


def draw_group_additional_shrinkage(key, part):
    place_key, loss_key = jax.random.split(jax.random.fold_in(key, 23))
    places = jax.random.randint(place_key, (FOCUS_GROUPS, 6), 0, CORPUS_SPAN)
    losses = jax.random.uniform(loss_key, (FOCUS_GROUPS, 6), jnp.float32, 0.2, 0.5)
    hits = jnp.arange(CORPUS_SPAN, dtype=jnp.int32)[:, None, None] == places[None, :, :]
    return jnp.sum(jnp.where(hits, jnp.log(1.0 - losses)[None], 0.0), axis=2).astype(jnp.float32)


def raised(array, rng, source, target, blocks, factor):
    def block_of(axis_at):
        return (jnp.arange(array.shape[axis_at]) // (array.shape[axis_at] // blocks)).reshape((-1,) + (1,) * (array.ndim - 1 - axis_at))

    first = jax.random.permutation(rng, blocks)[block_of(target)]
    other_side = (block_of(target) + blocks // 2) % blocks
    return jnp.where((block_of(source) == first) | (block_of(source) == other_side), factor * array, array)


def block_scale(key, extent, cuts, smallest, top_value):
    def one(dim, parts):
        steps = jax.random.uniform(jax.random.fold_in(jax.random.fold_in(key, 6), dim), (parts,), jnp.float32, smallest / len(cuts), top_value / len(cuts))
        return jnp.repeat(jnp.exp(steps), extent[dim] // parts).reshape((-1,) + (1,) * (len(extent) - dim - 1))

    gain = one(*cuts[0])
    for cut in cuts[1:]:
        gain = gain * one(*cut)
    return gain


def routed_block(own_key, own, number, rows, number_of, top, bound, skew):
    sequence = jax.random.permutation(own_key, number_of)
    crowded, ordinary = portions_of(number_of, rows * top, bound, skew, True), portions_of(number_of, rows * top, bound, skew, False)
    places = jnp.arange(number_of)

    def named(tallies, turn):
        used = int((tallies > 0).sum())
        fixed = max(1, used // 4)
        moved = fixed + (places - fixed + turn * (used - fixed)) % max(1, number_of - fixed)
        return jnp.zeros((number_of,), jnp.int32).at[sequence[jnp.where(places < fixed, places, moved)]].set(jnp.asarray(tallies, jnp.int32))

    tallies = jnp.where(number % 4 == 0, named(crowded, number // 4), named(ordinary, number - number // 4 - 1))
    mixed = jax.random.permutation(jax.random.fold_in(own, 3), number_of)
    donor, taker = mixed[0:number_of // 2 * 2:2], mixed[1:number_of // 2 * 2:2]
    room = jnp.minimum(tallies[donor] - 1, bound - tallies[taker]) // 2
    room = jnp.where((donor == sequence[0]) | (taker == sequence[0]) | (tallies[taker] == 0), 0, jnp.maximum(room, 0))
    moved = jax.random.randint(jax.random.fold_in(own, 4), (number_of // 2,), 0, 1 << 20) % (room + 1)
    tallies = tallies.at[donor].add(-moved).at[taker].add(moved)
    labels = jnp.searchsorted(jnp.cumsum(tallies), jnp.arange(rows * top), side="right").astype(jnp.int32)
    table = labels.reshape(top, rows).T
    table = table[jax.random.permutation(jax.random.fold_in(own, 1), rows)]
    turn = jax.random.randint(jax.random.fold_in(own, 2), (rows, 1), 0, top)
    return jnp.take_along_axis(table, (jnp.arange(top)[None, :] + turn) % top, axis=1)


def portions_of(count, total, most, slope, full):
    portions = [(1 << 20) // math.isqrt(standing ** slope) + 1 for standing in range(1, count + 1)]
    largest = most if full else min(most, max(-(-total // count), total * portions[0] // sum(portions)))
    least = 1 if total - largest >= count - 1 else 0
    given, surplus = [largest] + [least] * (count - 1), total - largest - least * (count - 1)
    while surplus > 0:
        movable = [i for i in range(1, count) if given[i] < largest] or [i for i in range(1, count) if given[i] < most]
        whole, budget = sum([portions[i] for i in movable]), surplus
        for i in movable:
            extra = min(most - given[i], max(1, budget * portions[i] // whole), surplus)
            given[i] = given[i] + extra
            surplus = surplus - extra
    return np.array(given)


def bell_draw(key, extent, scale, reach, cuts=(), held_as=jnp.bfloat16):
    drawn = jax.random.normal(key, extent, jnp.float32) * scale
    if len(cuts) > 0:
        drawn = block_scale(key, extent, cuts, -0.22, 0.18) * drawn
    return jnp.clip(drawn, min=-reach, max=reach).astype(held_as)


def gaussian_with(rng, dims, scale, reach, pieces, heavy, kind=jnp.bfloat16):
    drawn = scale * jax.random.normal(rng, dims, jnp.float32)
    if pieces:
        drawn = drawn * block_scale(rng, dims, pieces, -0.22, 0.18)
    return jnp.clip(raised(drawn, jax.random.fold_in(rng, 3), *heavy), -reach, reach).astype(kind)


def setup_inputs(seed: int = 0) -> dict:
    key_of = jax.random.split(jax.random.key(seed), 17)
    residual_signal = bell_draw(key_of[0], (CORPUS_SPAN, D), 1.0, 6.0, ((0, 512),))
    prelayer_scaling_factor = jnp.clip(1.0 + 0.18 * jax.random.normal(key_of[1], (D,), jnp.float32), 0.1, 1.9)
    result_adjoint = gaussian_with(key_of[2], (CORPUS_SPAN, D), 1.0, 24.0, ((0, 512),), (0, 1, 512, 6.0))
    chosen_specialist_ids_keys = jax.random.split(jax.random.fold_in(key_of[3], 1), CORPUS_SPAN // TOK_DEV)
    chosen_specialist_ids_turns = jax.random.permutation(jax.random.fold_in(key_of[3], 3), CORPUS_SPAN // TOK_DEV)
    chosen_specialist_ids = jax.vmap(lambda own, number: routed_block(jax.random.fold_in(key_of[3], 2), own, number, TOK_DEV, EXPERTS, TOP, CAP, 2))(chosen_specialist_ids_keys, chosen_specialist_ids_turns).reshape((CORPUS_SPAN, TOP))
    dispatch_shares = jnp.clip(0.2 + 0.8 * jax.random.uniform(key_of[4], (CORPUS_SPAN, TOP), jnp.float32) ** block_scale(key_of[4], (CORPUS_SPAN, TOP), ((0, 32),), -0.2, 0.2), 0.2, 1.0)
    specialist_valve_matrix = bell_draw(key_of[5], (EXPERTS, D, FF), D ** -0.5, 0.125, ((0, 32), (2, 16)))
    specialist_widen_matrix = bell_draw(key_of[6], (EXPERTS, D, FF), D ** -0.5, 0.125, ((0, 32), (2, 16)))
    specialist_shrink_matrix = bell_draw(key_of[7], (EXPERTS, FF, D), FF ** -0.5, 0.125, ((0, 32), (1, 16)))
    probe_vectors = bell_draw(key_of[8], (CORPUS_SPAN, QUERY_CHANNELS), 1.0, 6.0, ((0, 32),))
    lookup_vectors = bell_draw(key_of[9], (CORPUS_SPAN, QUERY_CHANNELS), 0.25, 1.5, ((0, 32),))
    persistence_scores = draw_persistence_scores(jax.random.fold_in(key_of[16], 71), 0)
    group_additional_shrinkage = draw_group_additional_shrinkage(jax.random.fold_in(key_of[16], 71), 0)
    content_vectors = bell_draw(key_of[12], (CORPUS_SPAN, FOCUS_GROUPS, HEAD_V), 1.0, 6.0, ((0, 32), (2, 16)))
    result_valve_scores = bell_draw(key_of[13], (CORPUS_SPAN, FOCUS_GROUPS, HEAD_V), 1.0, 6.0, ((0, 32), (2, 16)))
    stored_opening_memory = bell_draw(key_of[14], (N_SP, FOCUS_GROUPS, FEATURE_DIMS, HEAD_V), 4.0, 24.0, ((0, 32), (3, 16)), jnp.float32)
    result_mapping_matrix = bell_draw(key_of[15], (D, FOCUS_GROUPS, HEAD_V), (FOCUS_GROUPS * HEAD_V) ** -0.5, 0.125, ((2, 16),))
    return {"residual_signal": residual_signal, "prelayer_scaling_factor": prelayer_scaling_factor, "result_adjoint": result_adjoint, "chosen_specialist_ids": chosen_specialist_ids, "dispatch_shares": dispatch_shares, "specialist_valve_matrix": specialist_valve_matrix, "specialist_widen_matrix": specialist_widen_matrix, "specialist_shrink_matrix": specialist_shrink_matrix, "probe_vectors": probe_vectors, "lookup_vectors": lookup_vectors, "persistence_scores": persistence_scores, "group_additional_shrinkage": group_additional_shrinkage, "content_vectors": content_vectors, "result_valve_scores": result_valve_scores, "stored_opening_memory": stored_opening_memory, "result_mapping_matrix": result_mapping_matrix}


toggle_smoothness = 16.0
norm_eps = 1e-06

def silu_slope(value):
    sigma = jax.nn.sigmoid(value)
    return sigma + value * sigma * (1.0 - sigma)

def expert_rows(item, input_rows, cot_rows):
    w_gate, w_up, w_down, index = item
    inputs = input_rows[index]
    cotangent = cot_rows[index]
    contract_last = (((1,), (1,)), ((), ()))
    contract_first = (((0,), (0,)), ((), ()))
    pre_gate = jnp.dot(inputs, w_gate, preferred_element_type=jnp.float32)
    pre_up = jnp.dot(inputs, w_up, preferred_element_type=jnp.float32)
    hidden = (jax.nn.silu(pre_gate) * pre_up).astype(jnp.bfloat16)
    hidden_grad = lax.dot_general(cotangent, w_down, contract_last, preferred_element_type=jnp.float32)
    down_part = lax.dot_general(hidden, cotangent, contract_first, preferred_element_type=jnp.float32).astype(jnp.bfloat16)
    gate_pre = (hidden_grad * pre_up * silu_slope(pre_gate)).astype(jnp.bfloat16)
    up_pre = (hidden_grad * jax.nn.silu(pre_gate)).astype(jnp.bfloat16)
    gate_part = lax.dot_general(inputs, gate_pre, contract_first, preferred_element_type=jnp.float32).astype(jnp.bfloat16)
    up_part = lax.dot_general(inputs, up_pre, contract_first, preferred_element_type=jnp.float32).astype(jnp.bfloat16)
    row_count = inputs.shape[0]
    group_gate = gate_pre.astype(jnp.float32).reshape(row_count, N_TP, FF_PART)
    group_up = up_pre.astype(jnp.float32).reshape(row_count, N_TP, FF_PART)
    weight_gate = w_gate.astype(jnp.float32).reshape(D, N_TP, FF_PART)
    weight_up = w_up.astype(jnp.float32).reshape(D, N_TP, FF_PART)
    groups = jnp.einsum('rgf,dgf->grd', group_gate, weight_gate) + jnp.einsum('rgf,dgf->grd', group_up, weight_up)
    groups = lax.optimization_barrier(groups.astype(jnp.bfloat16))
    routed = lax.optimization_barrier(jnp.sum(groups.astype(jnp.float32), axis=0)).astype(jnp.bfloat16)
    return (routed, gate_part, up_part, down_part)

def reference(residual_signal, prelayer_scaling_factor, result_adjoint, chosen_specialist_ids, dispatch_shares, specialist_valve_matrix, specialist_widen_matrix, specialist_shrink_matrix, probe_vectors, lookup_vectors, persistence_scores, group_additional_shrinkage, content_vectors, result_valve_scores, stored_opening_memory, result_mapping_matrix):
    residual = residual_signal.astype(jnp.float32)
    inv_rms = lax.rsqrt(lax.optimization_barrier(jnp.mean(residual * residual, axis=1, keepdims=True)) + norm_eps)
    unit_rows = residual * inv_rms
    moe_input = (unit_rows * prelayer_scaling_factor).astype(jnp.bfloat16)
    weighted = (dispatch_shares[:, :, None] * result_adjoint.astype(jnp.float32)[:, None, :]).astype(jnp.bfloat16)
    span_ids = chosen_specialist_ids.reshape(N_SP, TOK_DEV * TOP)
    one_hot = (span_ids[:, :, None] == jnp.arange(EXPERTS, dtype=jnp.int32)[None, None, :]).astype(jnp.int32)
    slot_index = lax.optimization_barrier(jnp.sum((jnp.cumsum(one_hot, axis=1) - one_hot) * one_hot, axis=2))
    span_index = jnp.arange(N_SP, dtype=jnp.int32)[:, None]
    destination = (span_ids * (N_SP * CAP) + span_index * CAP + slot_index).reshape(-1)
    assigned = CORPUS_SPAN * TOP
    source_of = jnp.full((EXPERTS * N_SP * CAP,), assigned, jnp.int32).at[destination].set(jnp.arange(assigned, dtype=jnp.int32))
    zero_row = jnp.zeros((1, D), jnp.bfloat16)
    input_rows = jnp.concatenate([jnp.repeat(moe_input, TOP, axis=0), zero_row], axis=0)
    cot_rows = jnp.concatenate([weighted.reshape(assigned, D), zero_row], axis=0)
    routed, gate_grad, up_grad, down_grad = lax.map(lambda item: expert_rows(item, input_rows, cot_rows), (specialist_valve_matrix, specialist_widen_matrix, specialist_shrink_matrix, source_of.reshape(EXPERTS, N_SP * CAP)))
    picked = routed.reshape(EXPERTS * N_SP * CAP, D)[destination].astype(jnp.float32)
    input_grad = lax.optimization_barrier(jnp.sum(picked.reshape(CORPUS_SPAN, TOP, D), axis=1))
    scaled = prelayer_scaling_factor * input_grad
    stream_full = result_adjoint.astype(jnp.float32) + inv_rms * (scaled - unit_rows * lax.optimization_barrier(jnp.mean(scaled * unit_rows, axis=1, keepdims=True)))
    stream_grad = stream_full.astype(jnp.bfloat16)
    piece_ordinal = CORPUS_SPAN // PIECE_PLACES
    per_span = TOK_DEV // PIECE_PLACES
    query_scale = FEATURE_DIMS ** (-0.5)
    exponent_shrinkage = (jax.nn.log_sigmoid(persistence_scores.astype(jnp.float32)).reshape(CORPUS_SPAN, FOCUS_GROUPS, FEATURE_DIMS) / toggle_smoothness + group_additional_shrinkage[:, :, None]).reshape(piece_ordinal, PIECE_PLACES, FOCUS_GROUPS, FEATURE_DIMS)
    cumulative = jnp.cumsum(exponent_shrinkage, axis=1)
    totals = cumulative[:, -1]
    factor = jnp.exp(totals[:, None] - cumulative)
    key_weight = lookup_vectors.astype(jnp.float32).reshape(piece_ordinal, PIECE_PLACES, FOCUS_GROUPS, FEATURE_DIMS) * factor
    decayed = key_weight.astype(jnp.bfloat16)
    value_blocks = content_vectors.astype(jnp.float32).reshape(piece_ordinal, PIECE_PLACES, FOCUS_GROUPS, HEAD_V)
    scaled_query = probe_vectors.astype(jnp.float32).reshape(piece_ordinal, PIECE_PLACES, FOCUS_GROUPS, FEATURE_DIMS) * query_scale

    def to_spans(tensor):
        return tensor.reshape((N_SP, per_span) + tensor.shape[1:])

    def span_states(item):
        begin_state, span_totals, span_decayed, span_values = item

        def block_step(running_state, inputs):
            total_of_block, decayed_block_terms, value_rows_block = inputs
            updated_state = running_state * jnp.exp(total_of_block)[:, :, None] + jnp.einsum('yno,ynt->not', decayed_block_terms.astype(jnp.float32), value_rows_block)
            return (updated_state, (running_state, updated_state))
        unused, pair = lax.scan(block_step, begin_state, (span_totals, span_decayed, span_values))
        return pair
    priors, states = lax.map(span_states, (stored_opening_memory, to_spans(totals), to_spans(decayed), to_spans(value_blocks)))
    priors = priors.reshape(piece_ordinal, FOCUS_GROUPS, FEATURE_DIMS, HEAD_V)
    states = states.reshape(piece_ordinal, FOCUS_GROUPS, FEATURE_DIMS, HEAD_V)
    readout = jnp.einsum('bchk,bhkv->bchv', scaled_query, states).reshape(CORPUS_SPAN, FOCUS_GROUPS, HEAD_V)
    gated_grad = jnp.einsum('td,dhv->thv', stream_grad.astype(jnp.float32), result_mapping_matrix.astype(jnp.float32))
    gate_value = result_valve_scores.astype(jnp.float32)
    gate_silu = jax.nn.silu(gate_value)
    gated_rows = (readout * gate_silu).astype(jnp.bfloat16)
    proj_grad = jnp.einsum('td,thv->dhv', stream_grad.astype(jnp.float32), gated_rows.astype(jnp.float32))
    readout_grad = gated_grad * gate_silu
    gate_input_grad = (gated_grad * readout * silu_slope(gate_value)).astype(jnp.bfloat16)
    readout_blocks = readout_grad.reshape(piece_ordinal, PIECE_PLACES, FOCUS_GROUPS, HEAD_V)
    local_terms = jnp.einsum('bchk,bchv->bhkv', scaled_query, readout_blocks)

    def back_step(carried, inputs):
        block_local, total_of_block = inputs
        block_grad = block_local + carried
        return (block_grad * jnp.exp(total_of_block)[:, :, None], block_grad)
    unused, state_grad = lax.scan(back_step, jnp.zeros((FOCUS_GROUPS, FEATURE_DIMS, HEAD_V), jnp.float32), (local_terms, totals), reverse=True)
    value_grad = jnp.einsum('bchk,bhkv->bchv', decayed.astype(jnp.float32), state_grad).astype(jnp.bfloat16).reshape(CORPUS_SPAN, FOCUS_GROUPS, HEAD_V)
    decayed_grad = jnp.einsum('bchv,bhkv->bchk', value_blocks, state_grad)
    key_grad = (decayed_grad * factor).astype(jnp.bfloat16).reshape(CORPUS_SPAN, QUERY_CHANNELS)
    combined_derivative = lax.optimization_barrier(jnp.sum(priors * jnp.exp(totals)[:, :, :, None] * state_grad, axis=3))
    moved_terms = decayed_grad * key_weight
    preceding_cumulation = jnp.cumsum(moved_terms, axis=1) - moved_terms
    preact_segments = persistence_scores.astype(jnp.float32).reshape(piece_ordinal, PIECE_PLACES, FOCUS_GROUPS, FEATURE_DIMS)
    retain_preact_derivative = ((combined_derivative[:, None] + preceding_cumulation) * jax.nn.sigmoid(-preact_segments) / toggle_smoothness).reshape(CORPUS_SPAN, QUERY_CHANNELS)

    def query_block(item):
        block_grad, block_state = item
        groups = jnp.einsum('chgv,hkgv->gchk', block_grad.reshape(PIECE_PLACES, FOCUS_GROUPS, N_TP, HV_PART), block_state.reshape(FOCUS_GROUPS, FEATURE_DIMS, N_TP, HV_PART)) * query_scale
        groups = lax.optimization_barrier(groups.astype(jnp.bfloat16))
        return lax.optimization_barrier(jnp.sum(groups.astype(jnp.float32), axis=0)).astype(jnp.bfloat16)
    query_grad = lax.map(query_block, (readout_blocks, states)).reshape(CORPUS_SPAN, QUERY_CHANNELS)
    return (stream_grad, gate_grad, up_grad, down_grad, proj_grad, query_grad, key_grad, retain_preact_derivative, value_grad, gate_input_grad)
```

```python
import jax
import jax.numpy as jnp
from jax import lax
from jax.sharding import Mesh
from jax.sharding import PartitionSpec as P

PIECE_PLACES = 64
SP = ("sp_0", "sp_1")
SP_TP = ("sp_0", "sp_1", "tp")


toggle_smoothness = 16.0
norm_eps = 1e-06


def from_everyone(shard, axis):
    copies = jnp.broadcast_to(shard, (lax.axis_size(axis), *shard.shape))
    return lax.all_to_all(copies, axis, split_axis=0, concat_axis=0, tiled=True)


def joined_along(tiles, dim):
    tiles = jnp.moveaxis(tiles, 0, dim)
    shape = tiles.shape
    return tiles.reshape(*shape[:dim], shape[dim] * shape[dim + 1], *shape[dim + 2 :])


def gather_directly(shard, axis, dim):
    tiles = from_everyone(shard, axis)
    return joined_along(tiles, dim)


def cut_along(shard, dim, length):
    shape = shard.shape
    tiles = shard.reshape(*shape[:dim], length, shape[dim] // length, *shape[dim + 1 :])
    return jnp.moveaxis(tiles, dim, 0)


def sum_at_owner(shard, axis, dim):
    length = lax.axis_size(axis)
    tiles = lax.all_to_all(cut_along(shard, dim, length), axis, 0, 0, tiled=True)
    return jnp.sum(tiles.astype(jnp.float32), axis=0)


def carried_in(decay, carried):
    length = lax.axis_size(SP)
    shape = carried.shape
    mine = shape[0] * shape[1] // length
    decays = lax.all_gather(decay.reshape(-1), SP)
    start = lax.axis_index(SP) * mine
    decays = lax.dynamic_slice_in_dim(decays, start, mine, 1)
    pieces = carried.astype(jnp.bfloat16).reshape(length, mine, shape[2])
    pieces = lax.all_to_all(pieces, SP, 0, 0, tiled=True).astype(jnp.float32)
    value = jnp.zeros_like(pieces[0])
    values = [value] * length
    for k in reversed(range(length - 1)):
        value = pieces[k + 1] + decays[k + 1][:, None] * value
        values[k] = value
    values = jnp.stack(values).astype(jnp.bfloat16)
    back = lax.all_to_all(values, SP, 0, 0, tiled=True)
    return back.reshape(shape).astype(jnp.float32)


def sum_packed(arrays, axis, dims):
    length = lax.axis_size(axis)
    tiles = [cut_along(a, dim, length) for a, dim in zip(arrays, dims)]
    lines = jnp.concatenate([b.reshape(length, -1, 128) for b in tiles], axis=1)
    line = jnp.sum(lax.all_to_all(lines, axis, 0, 0, tiled=True).astype(jnp.float32), axis=0)
    line, at, gathered = (line.reshape(-1), 0, [])
    for b in tiles:
        part = b[0]
        gathered.append(line[at : at + part.size].reshape(part.shape))
        at += part.size
    return tuple(gathered)


def silu_slope(value):
    sigma = jax.nn.sigmoid(value)
    return sigma + value * sigma * (1.0 - sigma)


def expert_backward(routed_rows, w_gate, w_up, w_down):
    inputs = routed_rows[:, 0]
    cotangent = routed_rows[:, 1]
    contract_last = (((1,), (1,)), ((), ()))
    contract_first = (((0,), (0,)), ((), ()))
    pre_gate = jnp.dot(inputs, w_gate, preferred_element_type=jnp.float32)
    pre_up = jnp.dot(inputs, w_up, preferred_element_type=jnp.float32)
    hidden = (jax.nn.silu(pre_gate) * pre_up).astype(jnp.bfloat16)
    hidden_grad = lax.dot_general(
        cotangent, w_down, contract_last, preferred_element_type=jnp.float32
    )
    down_part = lax.dot_general(
        hidden, cotangent, contract_first, preferred_element_type=jnp.float32
    ).astype(jnp.bfloat16)
    gate_pre = (hidden_grad * pre_up * silu_slope(pre_gate)).astype(jnp.bfloat16)
    up_pre = (hidden_grad * jax.nn.silu(pre_gate)).astype(jnp.bfloat16)
    gate_part = lax.dot_general(
        inputs, gate_pre, contract_first, preferred_element_type=jnp.float32
    ).astype(jnp.bfloat16)
    up_part = lax.dot_general(
        inputs, up_pre, contract_first, preferred_element_type=jnp.float32
    ).astype(jnp.bfloat16)
    partial_value = lax.dot_general(
        gate_pre, w_gate, contract_last, preferred_element_type=jnp.float32
    ) + lax.dot_general(up_pre, w_up, contract_last, preferred_element_type=jnp.float32)
    return (partial_value.astype(jnp.bfloat16), gate_part, up_part, down_part)


def on_device(
    residual_signal,
    prelayer_scaling_factor,
    result_adjoint,
    chosen_specialist_ids,
    dispatch_shares,
    specialist_valve_matrix,
    specialist_widen_matrix,
    specialist_shrink_matrix,
    probe_vectors,
    lookup_vectors,
    persistence_scores,
    group_additional_shrinkage,
    content_vectors,
    result_valve_scores,
    stored_opening_memory,
    result_mapping_matrix,
):
    tp_count = lax.axis_size("tp")
    sp_count = lax.axis_size(SP)
    tp_index = lax.axis_index("tp")
    own_rows = residual_signal.shape[0]
    model_width = residual_signal.shape[1]
    column_width = model_width // tp_count
    own_residual = residual_signal.astype(jnp.float32)
    inv_rms = lax.rsqrt(jnp.mean(own_residual * own_residual, axis=1, keepdims=True) + norm_eps)
    unit_rows = own_residual * inv_rms
    own_input = (unit_rows * prelayer_scaling_factor).astype(jnp.bfloat16)
    paired = jnp.stack([cut_along(own_input, 1, tp_count), cut_along(result_adjoint, 1, tp_count)], axis=2)
    paired = lax.all_to_all(paired.reshape(tp_count, own_rows, 2 * column_width), "tp", 0, 0, tiled=True)
    paired = paired.reshape(tp_count * own_rows, 2 * column_width)
    input_table = paired[:, :column_width]
    cotangent = paired[:, column_width:]
    span_tokens = paired.shape[0]
    top_count = chosen_specialist_ids.shape[1]
    weighted = (dispatch_shares[:, :, None] * cotangent.astype(jnp.float32)[:, None, :]).astype(
        jnp.bfloat16
    )
    local_experts = specialist_valve_matrix.shape[0]
    expert_total = local_experts * sp_count
    assigned = span_tokens * top_count
    capacity = assigned // expert_total + assigned // (4 * expert_total)
    flat_ids = chosen_specialist_ids.reshape(assigned)
    one_hot = (flat_ids[:, None] == jnp.arange(expert_total, dtype=jnp.int32)[None, :]).astype(
        jnp.int32
    )
    slot_index = jnp.sum((jnp.cumsum(one_hot, axis=0) - one_hot) * one_hot, axis=1)
    destination = flat_ids * capacity + slot_index
    source_of = (
        jnp.full((expert_total * capacity,), assigned, jnp.int32)
        .at[destination]
        .set(jnp.arange(assigned, dtype=jnp.int32))
    )
    cot_table = weighted.reshape(assigned, column_width)
    input_table = jnp.concatenate([input_table, jnp.zeros((1, column_width), jnp.bfloat16)], axis=0)
    cot_table = jnp.concatenate([cot_table, jnp.zeros((1, column_width), jnp.bfloat16)], axis=0)
    outgoing = jnp.concatenate([input_table[source_of // top_count], cot_table[source_of]], axis=1)
    outgoing = outgoing.reshape(expert_total, capacity, 2 * column_width)
    arrived = lax.all_to_all(outgoing, SP, split_axis=0, concat_axis=0, tiled=True)
    arrived = from_everyone(arrived, "tp").reshape(
        tp_count, sp_count * capacity, 2, column_width
    )
    arrived = jnp.transpose(arrived, (1, 2, 0, 3)).reshape(sp_count, capacity, 2, model_width)
    by_expert = jnp.moveaxis(
        arrived.reshape(sp_count, local_experts, capacity, 2, model_width), 1, 0
    )
    by_expert = by_expert.reshape(local_experts, sp_count * capacity, 2, model_width)
    partial_value, gate_grad, up_grad, down_grad = jax.vmap(expert_backward)(
        by_expert, specialist_valve_matrix, specialist_widen_matrix, specialist_shrink_matrix
    )
    partial_value = jnp.moveaxis(
        partial_value.reshape(local_experts, sp_count, capacity, model_width), 0, 1
    )
    partial_value = partial_value.reshape(sp_count * local_experts, capacity, model_width)
    summed = sum_at_owner(partial_value, "tp", 2).astype(jnp.bfloat16)
    returned = lax.all_to_all(summed, SP, split_axis=0, concat_axis=0, tiled=True)
    picked = returned.reshape(expert_total * capacity, column_width)[destination].astype(
        jnp.float32
    )
    grad_columns = jnp.sum(picked.reshape(span_tokens, top_count, column_width), axis=1)
    input_grad = lax.all_to_all(
        grad_columns.astype(jnp.bfloat16).reshape(tp_count, own_rows, column_width), "tp", 0, 0, tiled=True
    )
    input_grad = joined_along(input_grad, 1).astype(jnp.float32)
    scaled = prelayer_scaling_factor * input_grad
    stream_grad = (
        result_adjoint.astype(jnp.float32)
        + inv_rms * (scaled - unit_rows * jnp.mean(scaled * unit_rows, axis=1, keepdims=True))
    ).astype(jnp.bfloat16)
    stream_full = gather_directly(stream_grad, "tp", 0)
    parallel_groups = group_additional_shrinkage.shape[1]
    key_width = probe_vectors.shape[1]
    head_key = key_width // parallel_groups
    value_part = content_vectors.shape[2]
    blocks = span_tokens // PIECE_PLACES
    query_scale = head_key ** (-0.5)

    def to_blocks(tensor):
        return tensor.reshape((blocks, PIECE_PLACES) + tensor.shape[1:])

    exponent_shrinkage = (
        jax.nn.log_sigmoid(persistence_scores.astype(jnp.float32)).reshape(
            span_tokens, parallel_groups, head_key
        )
        / toggle_smoothness
        + group_additional_shrinkage[:, :, None]
    )
    cumulative = jnp.cumsum(to_blocks(exponent_shrinkage), axis=1)
    totals = cumulative[:, -1]
    factor = jnp.exp(totals[:, None] - cumulative)
    key_weight = (
        to_blocks(lookup_vectors.reshape(span_tokens, parallel_groups, head_key)).astype(
            jnp.float32
        )
        * factor
    )
    decayed = key_weight.astype(jnp.bfloat16)
    value_blocks = to_blocks(content_vectors)
    block_terms = jnp.einsum(
        "bchk,bchv->bhkv", decayed, value_blocks, preferred_element_type=jnp.float32
    )
    running_state = stored_opening_memory[0]
    prior_list = []
    state_list = []
    for block_index in range(blocks):
        prior_list.append(running_state)
        running_state = (
            running_state * jnp.exp(totals[block_index])[:, :, None] + block_terms[block_index]
        )
        state_list.append(running_state)
    priors = jnp.stack(prior_list)
    states = jnp.stack(state_list)
    scaled_query = (
        to_blocks(probe_vectors.reshape(span_tokens, parallel_groups, head_key)).astype(jnp.float32)
        * query_scale
    )
    readout = jnp.einsum("bchk,bhkv->bchv", scaled_query, states).reshape(
        span_tokens, parallel_groups, value_part
    )
    gated_grad = jnp.dot(
        stream_full,
        result_mapping_matrix.reshape(model_width, parallel_groups * value_part),
        preferred_element_type=jnp.float32,
    ).reshape(span_tokens, parallel_groups, value_part)
    gate_value = result_valve_scores.astype(jnp.float32)
    gate_silu = jax.nn.silu(gate_value)
    gated_flat = (
        (readout * gate_silu)
        .astype(jnp.bfloat16)
        .reshape(span_tokens, parallel_groups * value_part)
    )
    product = lax.dot_general(
        stream_full, gated_flat, (((0,), (0,)), ((), ())), preferred_element_type=jnp.float32
    )
    proj_grad = sum_at_owner(
        product.reshape(
            model_width // sp_count * lax.axis_size(SP), parallel_groups, value_part
        ).astype(jnp.bfloat16),
        SP,
        0,
    )
    readout_grad = gated_grad * gate_silu
    gate_input_grad = (gated_grad * readout * silu_slope(gate_value)).astype(jnp.bfloat16)
    readout_blocks = to_blocks(readout_grad)
    local_terms = jnp.einsum("bchk,bchv->bhkv", scaled_query, readout_blocks)
    carried = jnp.zeros_like(running_state)
    local_list = [carried] * blocks
    for block_index in reversed(range(blocks)):
        local_list[block_index] = local_terms[block_index] + carried
        carried = local_list[block_index] * jnp.exp(totals[block_index])[:, :, None]
    local_grads = jnp.stack(local_list)
    span_total = jnp.sum(totals, axis=0)
    span_decay = jnp.exp(span_total)
    incoming = carried_in(span_decay, carried)
    tail_sum = span_total[None] - jnp.cumsum(totals, axis=0)
    state_grad = local_grads + jnp.exp(tail_sum)[..., None] * incoming[None]
    value_grad = (
        jnp.einsum("bchk,bhkv->bchv", decayed.astype(jnp.float32), state_grad)
        .astype(jnp.bfloat16)
        .reshape(span_tokens, parallel_groups, value_part)
    )
    decayed_grad = jnp.einsum("bchv,bhkv->bchk", value_blocks.astype(jnp.float32), state_grad)
    combined_derivative = jnp.sum(priors * jnp.exp(totals)[..., None] * state_grad, axis=3)
    query_part = (jnp.einsum("bchv,bhkv->bchk", readout_blocks, states) * query_scale).astype(
        jnp.bfloat16
    )
    query_grad = sum_at_owner(query_part.reshape(span_tokens, key_width), "tp", 1).astype(
        jnp.bfloat16
    )
    key_sums, total_sums = tuple(
        (
            part.astype(jnp.float32)
            for part in sum_packed(
                (
                    decayed_grad.reshape(span_tokens, key_width).astype(jnp.bfloat16),
                    combined_derivative.reshape(blocks, key_width).astype(jnp.bfloat16),
                ),
                "tp",
                (1, 1),
            )
        )
    )
    own_width = key_width // tp_count
    own_start = tp_index * own_width

    def own_columns(tensor):
        return lax.dynamic_slice_in_dim(
            tensor.reshape(span_tokens, key_width), own_start, own_width, 1
        )

    key_grad = (key_sums * own_columns(factor)).astype(jnp.bfloat16)
    moved_terms = (key_sums * own_columns(key_weight)).reshape(blocks, PIECE_PLACES, own_width)
    preceding_cumulation = jnp.cumsum(moved_terms, axis=1) - moved_terms
    logit_own = own_columns(persistence_scores.astype(jnp.float32))
    retain_preact_derivative = (
        (total_sums[:, None] + preceding_cumulation).reshape(span_tokens, own_width)
        * jax.nn.sigmoid(-logit_own)
        / toggle_smoothness
    )
    return (
        stream_grad,
        gate_grad,
        up_grad,
        down_grad,
        proj_grad,
        query_grad,
        key_grad,
        retain_preact_derivative,
        value_grad,
        gate_input_grad,
    )


def solution(mesh):
    finer = Mesh(mesh.devices.reshape(16, 2, mesh.shape["tp"]), ("sp_0", "sp_1", "tp"))
    in_specs = (
        P(SP_TP, None),
        P(),
        P(SP_TP, None),
        P(SP, None),
        P(SP, None),
        P(SP, None, "tp"),
        P(SP, None, "tp"),
        P(SP, "tp", None),
        P(SP, None),
        P(SP, None),
        P(SP, None),
        P(SP, None),
        P(SP, None, "tp"),
        P(SP, None, "tp"),
        P(SP, None, None, "tp"),
        P(None, None, "tp"),
    )
    out_specs = (
        P(SP_TP, None),
        P(SP, None, "tp"),
        P(SP, None, "tp"),
        P(SP, "tp", None),
        P(SP, None, "tp"),
        P(SP, "tp"),
        P(SP, "tp"),
        P(SP, "tp"),
        P(SP, None, "tp"),
        P(SP, None, "tp"),
    )
    return jax.shard_map(
        on_device, mesh=finer, in_specs=in_specs, out_specs=out_specs, check_vma=False
    )
```

```python
import jax
import jax.numpy as jnp
from jax import lax
from jax.experimental import pallas as pl
from jax.experimental.pallas import tpu as pltpu
from jax.sharding import PartitionSpec as P

MESH = pl.DeviceIdType.MESH
F32 = jnp.float32
BF16 = jnp.bfloat16
HIGHEST = lax.Precision.HIGHEST

BLOCK = 64
TOGGLE = 16.0
EPS = 1e-06
PITCH = 16


def iota(shape, dim):
    return lax.broadcasted_iota(jnp.int32, shape, dim)


def dot(a, b):
    return jnp.dot(a, b, preferred_element_type=F32)


def dot_nt(a, b):
    return lax.dot_general(a, b, (((1,), (1,)), ((), ())), preferred_element_type=F32)


def dot_tn(a, b):
    return lax.dot_general(a, b, (((0,), (0,)), ((), ())), preferred_element_type=F32)


def silu_slope(value, sigma):
    return sigma + value * sigma * (1.0 - sigma)


def peer(me, i, n):
    half = n // 2
    up = half - i // 2
    offset = jnp.where(i % 2 == 0, up, n - up + 1)
    return lax.rem(me + offset, n)


def kernel(
    n_sp,
    n_tp,
    cap,
    res_ref,
    cot_ref,
    gain_ref,
    ids_row_ref,
    share_ref,
    wg_ref,
    wu_ref,
    wd_ref,
    q_ref,
    k_ref,
    pers_ref,
    shrink_ref,
    val_ref,
    valve_ref,
    mem_ref,
    map_ref,
    stream_out,
    gate_out,
    up_out,
    down_out,
    proj_out,
    query_out,
    key_out,
    retain_out,
    value_out,
    gig_out,
    p0_send,
    p0_recv,
    dec_all,
    p1_send,
    p1_recv,
    cx,
    cw,
    x_all,
    w_all,
    wgu,
    rs_send,
    rs_recv,
    ret_send,
    ret_recv,
    ig_send,
    ig_recv,
    st_send,
    st_recv,
    sc_send,
    sc_recv,
    bk_send,
    bk_recv,
    pj_local,
    pj_away,
    pj_partner,
    pj_send,
    pj_recv,
    q_send,
    q_recv,
    k_send,
    k_recv,
    m_sum,
    factor_ref,
    kw_ref,
    states,
    readout_ref,
    local_ref,
    sf_ref,
    gup_ref,
    hid_ref,
    ssem,
    rsem,
):
    sp = lax.axis_index("sp")
    tp = lax.axis_index("tp")
    core = lax.rem(sp, 2)
    own_rows, width = res_ref.shape
    tokens = own_rows * n_tp
    rows = n_sp * cap
    padded = n_sp * PITCH
    head_k = q_ref.shape[1] // 2

    barrier = pltpu.get_barrier_semaphore()

    def greet(axis, me, n):
        def body(i, carry):
            pl.semaphore_signal(
                barrier, inc=1, device_id={axis: peer(me, i, n)}, device_id_type=MESH
            )
            return carry

        lax.fori_loop(0, n - 1, body, 0)

    greet("sp", sp, n_sp)
    greet("tp", tp, n_tp)

    def copy(src, dst, slot, device):
        return pltpu.make_async_remote_copy(
            src_ref=src,
            dst_ref=dst,
            send_sem=ssem.at[slot],
            recv_sem=rsem.at[slot],
            device_id=device,
            device_id_type=MESH,
        )

    def spread(axis, me, n, slot, src_of, dst):
        def body(i, carry):
            p = peer(me, i, n)
            copy(src_of(p), dst, slot, {axis: p}).start()
            return carry

        lax.fori_loop(0, n - 1, body, 0)

    def received(slot, part):
        copy(part, part, slot, {"tp": lax.rem(tp + 1, n_tp)}).wait_recv()

    def sent(slot, part):
        copy(part, part, slot, {"tp": lax.rem(tp + 1, n_tp)}).wait_send()

    residual = res_ref[...].astype(F32)
    own_cot = cot_ref[...]
    inv_rms = lax.rsqrt(jnp.mean(residual * residual, axis=1, keepdims=True) + EPS)
    unit = residual * inv_rms
    own_input = (unit * gain_ref[...]).astype(BF16)
    for j in range(n_tp):
        p0_send[j, :, 0:128] = own_input[:, 128 * j : 128 * (j + 1)]
        p0_send[j, :, 128:256] = own_cot[:, 128 * j : 128 * (j + 1)]
    p0_recv[tp] = p0_send[tp]

    pl.semaphore_wait(barrier, (n_sp - 1) + (n_tp - 1))
    spread("tp", tp, n_tp, 0, lambda p: p0_send.at[p], p0_recv.at[tp])

    spot = iota((padded, tokens), 0)
    expert_rows = iota((n_sp, tokens), 0)
    earlier = (iota((tokens, tokens), 0) < iota((tokens, tokens), 1)).astype(BF16)
    ids0 = ids_row_ref[0:1, :]
    ids1 = ids_row_ref[1:2, :]
    hot0 = (expert_rows == ids0).astype(F32)
    hot1 = (expert_rows == ids1).astype(F32)
    counts = dot((hot0 + hot1).astype(BF16), earlier)
    slot0 = jnp.sum(hot0 * counts, axis=0, keepdims=True).astype(jnp.int32)
    slot1 = jnp.sum(hot1 * counts, axis=0, keepdims=True).astype(jnp.int32)
    pick0 = (spot == ids0 * PITCH + slot0).astype(F32).astype(BF16)
    pick1 = (spot == ids1 * PITCH + slot1).astype(F32).astype(BF16)
    m_sum[...] = pick0 + pick1

    received(0, p0_recv.at[pl.ds(0, n_tp - 1)])
    table = p0_recv[...].astype(F32).reshape(tokens, 256)
    cot_table = table[:, 128:256]
    weighted0 = (share_ref[:, 0:1] * cot_table).astype(BF16)
    weighted1 = (share_ref[:, 1:2] * cot_table).astype(BF16)
    p1_send[:, :, 0:128] = (
        dot(m_sum[...], table[:, 0:128].astype(BF16)).astype(BF16).reshape(n_sp, PITCH, 128)
    )
    p1_send[:, :, 128:256] = (
        (dot(pick0, weighted0) + dot(pick1, weighted1)).astype(BF16).reshape(n_sp, PITCH, 128)
    )
    p1_recv[sp] = p1_send[sp]
    spread("sp", sp, n_sp, 1, lambda p: p1_send.at[p], p1_recv.at[sp])

    log_decay = pers_ref[...].astype(F32)
    log_decay = (jnp.minimum(log_decay, 0.0) - jnp.log1p(jnp.exp(-jnp.abs(log_decay)))) / TOGGLE
    left = iota((tokens, 2 * head_k), 1) < head_k
    log_decay = log_decay + jnp.where(left, shrink_ref[:, 0:1], shrink_ref[:, 1:2])
    row_id = iota((tokens, tokens), 0)
    col_id = iota((tokens, tokens), 1)
    after = ((col_id > row_id) & (col_id // BLOCK == row_id // BLOCK)).astype(F32)
    factor = jnp.exp(
        jnp.dot(after, log_decay, preferred_element_type=F32, precision=HIGHEST)
    )
    factor_ref[...] = factor
    total0 = jnp.sum(log_decay[0:BLOCK], axis=0, keepdims=True)
    total1 = jnp.sum(log_decay[BLOCK : 2 * BLOCK], axis=0, keepdims=True)
    etot0 = jnp.exp(total0)
    etot1 = jnp.exp(total1)
    span_decay = jnp.exp(total0 + total1)
    for j in range(8):
        dec_all[sp, j : j + 1, :] = span_decay[:, 128 * j : 128 * (j + 1)]
    spread("sp", sp, n_sp, 2, lambda p: dec_all.at[sp], dec_all.at[sp])
    key_weight = k_ref[...].astype(F32) * factor
    kw_ref[...] = key_weight
    wgu[:, 0:128] = wg_ref[...]
    wgu[:, 128:256] = wu_ref[...]

    received(1, p1_recv.at[pl.ds(0, n_sp - 1)])
    r_i = iota((rows, padded), 0)
    q_i = iota((rows, padded), 1)
    tight = ((q_i & (PITCH - 1)) < cap) & (r_i == (q_i // PITCH) * cap + (q_i & (PITCH - 1)))
    tight = tight.astype(F32).astype(BF16)
    compact = dot(tight, p1_recv[...].reshape(padded, 256)).astype(BF16)
    cx[...] = compact[:, 0:128]
    cw[...] = compact[:, 128:256]
    own_lanes = pl.ds(pl.multiple_of(tp * 128, 128), 128)
    spread("tp", tp, n_tp, 3, lambda p: cx, x_all.at[:, own_lanes])
    spread("tp", tp, n_tp, 4, lambda p: cw, w_all.at[:, own_lanes])
    x_all[:, own_lanes] = compact[:, 0:128]
    w_all[:, own_lanes] = compact[:, 128:256]

    scale = float(head_k) ** (-0.5)
    decayed = key_weight.astype(BF16)
    values_t = val_ref[...].astype(F32).T
    tok_block = iota((128, tokens), 1) // BLOCK
    etots = (etot0, etot1)
    for b in range(2):
        masked = jnp.where(tok_block == b, values_t, 0.0).astype(BF16)
        for h in range(2):
            term = dot(masked[64 * h : 64 * (h + 1)], decayed[:, head_k * h : head_k * (h + 1)])
            if b == 0:
                prior = mem_ref[64 * h : 64 * (h + 1), :]
            else:
                prior = states[0, 64 * h : 64 * (h + 1), :]
            states[b, 64 * h : 64 * (h + 1), :] = (
                prior * etots[b][:, head_k * h : head_k * (h + 1)] + term
            )
    first_head = iota((BLOCK, 128), 1) < 64

    def per_head(a, m, b):
        part = [
            dot_nt(a[BLOCK * b : BLOCK * (b + 1), head_k * h : head_k * (h + 1)], m)
            for h in range(2)
        ]
        return jnp.where(first_head, part[0], part[1])

    for b in range(2):
        readout_ref[BLOCK * b : BLOCK * (b + 1), :] = (
            per_head(q_ref[...], states[b].astype(BF16), b) * scale
        )

    received(3, x_all.at[:, pl.ds(0, 128 * (n_tp - 1))])
    received(4, w_all.at[:, pl.ds(0, 128 * (n_tp - 1))])
    pre = dot(x_all[...], wgu[...])
    pre_gate = pre[:, 0:128]
    pre_up = pre[:, 128:256]
    hidden_grad = dot_nt(w_all[...], wd_ref[...])
    sigma = jax.nn.sigmoid(pre_gate)
    silu = pre_gate * sigma
    gup_ref[:, 0:128] = (hidden_grad * pre_up * silu_slope(pre_gate, sigma)).astype(BF16)
    gup_ref[:, 128:256] = (hidden_grad * silu).astype(BF16)
    hid_ref[...] = (silu * pre_up).astype(BF16)

    def partial_of(p):
        return dot_nt(
            gup_ref[...], wgu[pl.ds(pl.multiple_of(p * 128, 128), 128), :]
        ).astype(BF16)

    def send_partial(i, carry):
        p = peer(tp, i, n_tp)
        rs_send[p] = partial_of(p)
        copy(rs_send.at[p], rs_recv.at[tp], 5, {"tp": p}).start()
        return carry

    lax.fori_loop(0, n_tp - 1, send_partial, 0)
    rs_recv[tp] = partial_of(tp)

    for j in range(width // 256):
        lanes = slice(256 * j, 256 * (j + 1))
        both = dot_tn(x_all[:, lanes], gup_ref[...])
        gate_out[lanes, :] = both[:, 0:128].astype(BF16)
        up_out[lanes, :] = both[:, 128:256].astype(BF16)
    down_out[...] = dot_tn(hid_ref[...], w_all[...]).astype(BF16)

    received(5, rs_recv.at[pl.ds(0, n_tp - 1)])
    summed = rs_recv[0].astype(F32)
    for j in range(1, n_tp):
        summed = summed + rs_recv[j].astype(F32)
    q_i = iota((padded, rows), 0)
    r_i = iota((padded, rows), 1)
    loose = ((q_i & (PITCH - 1)) < cap) & (r_i == (q_i // PITCH) * cap + (q_i & (PITCH - 1)))
    loose = loose.astype(F32).astype(BF16)
    ret_send[...] = dot(loose, summed.astype(BF16)).astype(BF16).reshape(n_sp, PITCH, 128)
    ret_recv[sp] = ret_send[sp]
    spread("sp", sp, n_sp, 6, lambda p: ret_send.at[p], ret_recv.at[sp])
    received(6, ret_recv.at[pl.ds(0, n_sp - 1)])

    picked = dot_tn(m_sum[...], ret_recv[...].reshape(padded, 128))
    ig_send[...] = picked.reshape(n_tp, own_rows, 128).astype(BF16)
    ig_recv[tp] = ig_send[tp]
    spread("tp", tp, n_tp, 7, lambda p: ig_send.at[p], ig_recv.at[tp])
    received(7, ig_recv.at[pl.ds(0, n_tp - 1)])
    input_grad = jnp.concatenate([ig_recv[j].astype(F32) for j in range(n_tp)], axis=1)
    scaled = gain_ref[...] * input_grad
    stream = (
        own_cot.astype(F32)
        + inv_rms * (scaled - unit * jnp.mean(scaled * unit, axis=1, keepdims=True))
    ).astype(BF16)
    stream_out[...] = stream
    st_send[...] = stream
    st_recv[tp] = stream
    spread("tp", tp, n_tp, 8, lambda p: st_send, st_recv.at[tp])
    received(8, st_recv.at[pl.ds(0, n_tp - 1)])
    sf_ref[...] = st_recv[...].astype(F32).reshape(tokens, width).astype(BF16)

    gated_grad = dot(sf_ref[...], map_ref[...])
    gate_value = valve_ref[...].astype(F32)
    gate_sigma = jax.nn.sigmoid(gate_value)
    gate_silu = gate_value * gate_sigma
    readout_grad = gated_grad * gate_silu
    rg = readout_grad.astype(BF16)
    rg_t = readout_grad.T
    for b in range(1, -1, -1):
        masked = jnp.where(tok_block == b, rg_t, 0.0).astype(BF16)
        for h in range(2):
            hs = slice(64 * h, 64 * (h + 1))
            ks = slice(head_k * h, head_k * (h + 1))
            term = dot(masked[hs], q_ref[:, ks]) * scale
            if b == 0:
                term = term + local_ref[1, hs, :] * etot1[:, ks]
            local_ref[b, hs, :] = term
            if b == 0:
                out = (term * etot0[:, ks]).astype(BF16)
                for r in range(4):
                    for c in range(4):
                        sc_send[(4 * h + r) * 4 + c] = out[
                            16 * r : 16 * (r + 1), 128 * c : 128 * (c + 1)
                        ]
    sc_recv[sp] = sc_send[sp]
    spread("sp", sp, n_sp, 9, lambda p: sc_send.at[p], sc_recv.at[sp])

    readout = readout_ref[...]
    gig_out[...] = (gated_grad * readout * silu_slope(gate_value, gate_sigma)).astype(BF16)
    gated = (readout * gate_silu).astype(BF16)
    partner = sp + 1 - 2 * core
    for j in range(width // 256):
        lanes = slice(256 * j, 256 * (j + 1))
        part = dot_tn(sf_ref[:, lanes], gated).astype(BF16)
        for i in range(2):
            z = 2 * j + i
            lower = part[128 * i : 128 * i + 64]
            upper = part[128 * i + 64 : 128 * i + 128]
            pj_local[z] = jnp.where(core == 0, lower, upper)
            pj_away[z] = jnp.where(core == 0, upper, lower)
    copy(pj_away, pj_partner, 10, {"sp": partner}).start()

    lower_lanes = iota((BLOCK, 128), 1) < 64

    def swap(a):
        return jnp.concatenate([a[:, 64:128], a[:, 0:64]], axis=1)

    def even_of(a, b):
        return jnp.where(lower_lanes[0 : a.shape[0]], a, swap(b))

    def odd_of(a, b):
        return jnp.where(lower_lanes[0 : a.shape[0]], swap(a), b)

    def by_head(a, m, h):
        keep = first_head if h == 0 else jnp.logical_not(first_head)
        return dot(jnp.where(keep, a.astype(F32), 0.0).astype(BF16), m)

    for h in range(2):
        part = [
            by_head(rg[BLOCK * b : BLOCK * (b + 1)], states[b].astype(BF16), h) * scale
            for b in range(2)
        ]
        for m in range(4):
            ls = slice(128 * m, 128 * (m + 1))
            q_send[8 * h + 2 * m] = even_of(part[0][:, ls], part[1][:, ls]).astype(BF16)
            q_send[8 * h + 2 * m + 1] = odd_of(part[0][:, ls], part[1][:, ls]).astype(BF16)
    q_recv[tp] = q_send[tp]
    spread("tp", tp, n_tp, 11, lambda p: q_send.at[p], q_recv.at[tp])

    received(2, dec_all.at[pl.ds(0, n_sp - 1)])
    received(9, sc_recv.at[pl.ds(0, n_sp - 1)])
    group = (sp // 16) * 4 + lax.rem(sp, 4)
    run = jnp.zeros((16, 128), F32)
    bk_send[n_sp - 1] = run.astype(BF16)
    for s in range(n_sp - 1, 0, -1):
        run = sc_recv[s].astype(F32) + dec_all[s, pl.ds(group, 1), :] * run
        bk_send[s - 1] = run.astype(BF16)
    bk_recv[sp] = bk_send[sp]
    spread("sp", sp, n_sp, 12, lambda p: bk_send.at[p], bk_recv.at[sp])

    received(10, pj_partner)
    pj_send[...] = (pj_local[...].astype(F32) + pj_partner[...].astype(F32)).astype(BF16)
    chip = sp // 2
    n_z = n_sp // 2

    def send_proj(i, carry):
        p = peer(chip, i, n_z)
        copy(pj_send.at[p], pj_recv.at[chip], 13, {"sp": 2 * p + core}).start()
        return carry

    lax.fori_loop(0, n_z - 1, send_proj, 0)
    pj_recv[chip] = pj_send[chip]

    received(12, bk_recv.at[pl.ds(0, n_sp - 1)])
    incoming = jnp.concatenate(
        [
            jnp.concatenate([bk_recv[4 * r + c].astype(F32) for c in range(4)], axis=1)
            for r in range(8)
        ],
        axis=0,
    )
    weight = jnp.concatenate(
        [
            jnp.broadcast_to(etot1[:, 0:head_k], (64, head_k)),
            jnp.broadcast_to(etot1[:, head_k : 2 * head_k], (64, head_k)),
        ],
        axis=0,
    )
    local_ref[1] = local_ref[1] + incoming
    local_ref[0] = local_ref[0] + weight * incoming
    grads = [local_ref[b].astype(BF16) for b in range(2)]
    for h in range(2):
        part = [
            by_head(val_ref[BLOCK * b : BLOCK * (b + 1), :], grads[b], h) for b in range(2)
        ]
        sums = []
        for b in range(2):
            hs = slice(64 * h, 64 * (h + 1))
            prior = mem_ref[hs, :] if b == 0 else states[0, hs, :]
            sums.append(
                jnp.sum(prior * local_ref[b, hs, :], axis=0, keepdims=True)
                * etots[b][:, head_k * h : head_k * (h + 1)]
            )
        for m in range(4):
            ls = slice(128 * m, 128 * (m + 1))
            for odd, of in ((0, even_of), (1, odd_of)):
                p = 8 * h + 2 * m + odd
                k_send[p, 0:BLOCK, :] = of(part[0][:, ls], part[1][:, ls]).astype(BF16)
                k_send[p, BLOCK : BLOCK + 16, :] = jnp.broadcast_to(
                    of(sums[0][:, ls], sums[1][:, ls]), (16, 128)
                ).astype(BF16)
    k_recv[tp] = k_send[tp]
    spread("tp", tp, n_tp, 14, lambda p: k_send.at[p], k_recv.at[tp])

    decayed = kw_ref[...].astype(BF16)
    for b in range(2):
        value_out[BLOCK * b : BLOCK * (b + 1), :] = per_head(decayed, grads[b], b).astype(BF16)

    def two_blocks(out, a):
        out[0:BLOCK, :] = a[:, 0:64].astype(out.dtype)
        out[BLOCK : 2 * BLOCK, :] = a[:, 64:128].astype(out.dtype)

    received(11, q_recv.at[pl.ds(0, n_tp - 1)])
    query = q_recv[0].astype(F32)
    for j in range(1, n_tp):
        query = query + q_recv[j].astype(F32)
    two_blocks(query_out, query)

    lanes = pl.ds(pl.multiple_of((tp // 2) * 128, 128), 128)
    is_odd = lax.rem(tp, 2) == 1

    def own_columns(ref):
        a = ref[0:BLOCK, lanes].astype(F32)
        b = ref[BLOCK : 2 * BLOCK, lanes].astype(F32)
        return jnp.where(is_odd, odd_of(a, b), even_of(a, b))

    own_factor = own_columns(factor_ref)
    own_weight = own_columns(kw_ref)
    slope = jax.nn.sigmoid(-own_columns(pers_ref)) / TOGGLE
    before = (iota((BLOCK, BLOCK), 0) > iota((BLOCK, BLOCK), 1)).astype(F32)

    received(14, k_recv.at[pl.ds(0, n_tp - 1)])
    keys = k_recv[0].astype(F32)
    for j in range(1, n_tp):
        keys = keys + k_recv[j].astype(F32)
    key_sum = keys[0:BLOCK]
    two_blocks(key_out, key_sum * own_factor)
    preceding = jnp.dot(
        before, key_sum * own_weight, preferred_element_type=F32, precision=HIGHEST
    )
    two_blocks(retain_out, (keys[BLOCK : BLOCK + 1] + preceding) * slope)

    received(13, pj_recv.at[pl.ds(0, n_z - 1)])
    proj = pj_recv[0].astype(F32)
    for j in range(1, n_z):
        proj = proj + pj_recv[j].astype(F32)
    proj_out[...] = proj

    sent(0, p0_send.at[pl.ds(0, n_tp - 1)])
    sent(1, p1_send.at[pl.ds(0, n_sp - 1)])
    sent(2, dec_all.at[pl.ds(0, n_sp - 1)])
    sent(3, x_all.at[:, pl.ds(0, 128 * (n_tp - 1))])
    sent(4, w_all.at[:, pl.ds(0, 128 * (n_tp - 1))])
    sent(5, rs_send.at[pl.ds(0, n_tp - 1)])
    sent(6, ret_send.at[pl.ds(0, n_sp - 1)])
    sent(7, ig_send.at[pl.ds(0, n_tp - 1)])
    sent(8, st_recv.at[pl.ds(0, n_tp - 1)])
    sent(9, sc_send.at[pl.ds(0, n_sp - 1)])
    sent(10, pj_away)
    sent(11, q_send.at[pl.ds(0, n_tp - 1)])
    sent(12, bk_send.at[pl.ds(0, n_sp - 1)])
    sent(13, pj_send.at[pl.ds(0, n_z - 1)])
    sent(14, k_send.at[pl.ds(0, n_tp - 1)])


def on_device(
    residual_signal,
    prelayer_scaling_factor,
    result_adjoint,
    chosen_specialist_ids,
    dispatch_shares,
    specialist_valve_matrix,
    specialist_widen_matrix,
    specialist_shrink_matrix,
    probe_vectors,
    lookup_vectors,
    persistence_scores,
    group_additional_shrinkage,
    content_vectors,
    result_valve_scores,
    stored_opening_memory,
    result_mapping_matrix,
):
    n_sp = lax.axis_size("sp")
    n_tp = lax.axis_size("tp")
    own_rows, width = residual_signal.shape
    tokens = own_rows * n_tp
    assigned = tokens * chosen_specialist_ids.shape[1]
    cap = assigned // n_sp + assigned // (4 * n_sp)
    rows = n_sp * cap
    padded = n_sp * PITCH
    head_k = probe_vectors.shape[1] // 2
    n_z = n_sp // 2

    args = (
        residual_signal,
        result_adjoint,
        prelayer_scaling_factor.reshape(1, width),
        chosen_specialist_ids.T,
        dispatch_shares,
        specialist_valve_matrix[0],
        specialist_widen_matrix[0],
        specialist_shrink_matrix[0],
        probe_vectors,
        lookup_vectors,
        persistence_scores,
        group_additional_shrinkage,
        content_vectors.reshape(tokens, 128),
        result_valve_scores.reshape(tokens, 128),
        jnp.swapaxes(stored_opening_memory[0], 1, 2).reshape(128, head_k),
        result_mapping_matrix.reshape(width, 128),
    )
    shape = jax.ShapeDtypeStruct
    outs = (
        shape((own_rows, width), BF16),
        shape((width, 128), BF16),
        shape((width, 128), BF16),
        shape((128, width), BF16),
        shape((64, 128), F32),
        shape((tokens, 64), BF16),
        shape((tokens, 64), BF16),
        shape((tokens, 64), F32),
        shape((tokens, 128), BF16),
        shape((tokens, 128), BF16),
    )
    vmem = pltpu.VMEM
    scratch = [
        vmem((n_tp, own_rows, 256), BF16),
        vmem((n_tp, own_rows, 256), BF16),
        vmem((n_sp, 8, 128), F32),
        vmem((n_sp, PITCH, 256), BF16),
        vmem((n_sp, PITCH, 256), BF16),
        vmem((rows, 128), BF16),
        vmem((rows, 128), BF16),
        vmem((rows, width), BF16),
        vmem((rows, width), BF16),
        vmem((width, 256), BF16),
        vmem((n_tp, rows, 128), BF16),
        vmem((n_tp, rows, 128), BF16),
        vmem((n_sp, PITCH, 128), BF16),
        vmem((n_sp, PITCH, 128), BF16),
        vmem((n_tp, own_rows, 128), BF16),
        vmem((n_tp, own_rows, 128), BF16),
        vmem((own_rows, width), BF16),
        vmem((n_tp, own_rows, width), BF16),
        vmem((n_sp, 16, 128), BF16),
        vmem((n_sp, 16, 128), BF16),
        vmem((n_sp, 16, 128), BF16),
        vmem((n_sp, 16, 128), BF16),
        vmem((n_z, 64, 128), BF16),
        vmem((n_z, 64, 128), BF16),
        vmem((n_z, 64, 128), BF16),
        vmem((n_z, 64, 128), BF16),
        vmem((n_z, 64, 128), BF16),
        vmem((n_tp, BLOCK, 128), BF16),
        vmem((n_tp, BLOCK, 128), BF16),
        vmem((n_tp, BLOCK + 16, 128), BF16),
        vmem((n_tp, BLOCK + 16, 128), BF16),
        vmem((padded, tokens), BF16),
        vmem((tokens, 2 * head_k), F32),
        vmem((tokens, 2 * head_k), F32),
        vmem((2, 128, head_k), F32),
        vmem((tokens, 128), F32),
        vmem((2, 128, head_k), F32),
        vmem((tokens, width), BF16),
        vmem((rows, 256), BF16),
        vmem((rows, 128), BF16),
        pltpu.SemaphoreType.DMA((15,)),
        pltpu.SemaphoreType.DMA((15,)),
    ]
    in_vmem = pl.BlockSpec(memory_space=pltpu.VMEM)

    def body(*refs):
        kernel(n_sp, n_tp, cap, *refs)

    results = pl.pallas_call(
        body,
        out_shape=outs,
        in_specs=[in_vmem] * len(args),
        out_specs=[in_vmem] * len(outs),
        scratch_shapes=scratch,
        compiler_params=pltpu.CompilerParams(
            collective_id=0, has_side_effects=True, vmem_limit_bytes=50 * 1024 * 1024
        ),
        name="layer_backward",
    )(*args)
    stream, gate, up, down, proj, query, key, retain, value, gig = results
    return (
        stream,
        gate[None],
        up[None],
        down[None],
        proj.reshape(64, 2, 64),
        query,
        key,
        retain,
        value.reshape(tokens, 2, 64),
        gig.reshape(tokens, 2, 64),
    )


def solution(mesh):
    both = ("sp", "tp")
    in_specs = (
        P(both, None),
        P(),
        P(both, None),
        P("sp", None),
        P("sp", None),
        P("sp", None, "tp"),
        P("sp", None, "tp"),
        P("sp", "tp", None),
        P("sp", None),
        P("sp", None),
        P("sp", None),
        P("sp", None),
        P("sp", None, "tp"),
        P("sp", None, "tp"),
        P("sp", None, None, "tp"),
        P(None, None, "tp"),
    )
    out_specs = (
        P(both, None),
        P("sp", None, "tp"),
        P("sp", None, "tp"),
        P("sp", "tp", None),
        P("sp", None, "tp"),
        P("sp", "tp"),
        P("sp", "tp"),
        P("sp", "tp"),
        P("sp", None, "tp"),
        P("sp", None, "tp"),
    )
    return jax.shard_map(
        on_device, mesh=mesh, in_specs=in_specs, out_specs=out_specs, check_vma=False
    )
```
